32 devices in a mesh: fs: 16 (over z, y, x), tp: 2 (over core).
Axes of the slice: x: 2, y: 2, z: 4, core: 2. Of those that a mesh axis runs over, the one named last changes fastest.
Arguments:
- normed_input: bfloat16 [8192, 2048], P('fs', 'tp'), may hold values from -6 to 6
- cotangent: bfloat16 [8192, 2048], P('fs', 'tp'), may hold values from -6 to 6
- up_weight: bfloat16 [2048, 8192], P('fs', 'tp'), may hold values from -0.125 to 0.125
- down_weight: bfloat16 [8192, 2048], P('tp', 'fs'), may hold values from -0.0625 to 0.0625
Outputs:
- input_grad: bfloat16 [8192, 2048], P('fs', 'tp')
- up_grad: float32 [2048, 8192], P('fs', 'tp')
- down_grad: float32 [8192, 2048], P('tp', 'fs')
The draws below stay inside these ranges and needn't reach their ends.
All inputs are finite; a program needn't handle non-finite values.
Results may differ from the reference program's by a relative error of at most 0.018.
Values may be sent and summed in bfloat16 or wider, within the bound.
A program may use at most 192 MiB of HBM per device.

```python
import jax
import jax.numpy as jnp
from jax import lax

D = 2048
FF = 8192
TOKENS = 8192
FF_BLOCKS = 2


def strengthened(array, key, source, target, blocks, factor):
    owner, partner = [(jnp.arange(array.shape[axis_at]) // (array.shape[axis_at] // blocks)).reshape([-1 if axis == axis_at else 1 for axis in range(array.ndim)]) for axis_at in (source, target)]
    chosen = jax.random.permutation(key, blocks)[partner]
    strong = (owner == chosen) | (owner == (partner + blocks // 2) % blocks)
    return jnp.where(strong, factor * array, array)


def steps_of(stream_key, extent, shards, smallest, top_value):
    gain = 1.0
    for position, shards_of in shards:
        steps = jax.random.uniform(jax.random.fold_in(jax.random.fold_in(stream_key, 6), position), (shards_of,), jnp.float32, smallest / len(shards), top_value / len(shards))
        gain = gain * jnp.repeat(jnp.exp(steps), extent[position] // shards_of).reshape((-1,) + (1,) * (len(extent) - 1 - position))
    return gain


def bell_draw(stream_key, dims, spread, limit, pieces=(), kind=jnp.bfloat16):
    array = spread * jax.random.normal(stream_key, dims, jnp.float32)
    if pieces:
        array = array * steps_of(stream_key, dims, pieces, -0.22, 0.18)
    return jnp.clip(array, -limit, limit).astype(kind)


def heavy_noise(own_key, extent, spread, limit, cuts, heavy, kind=jnp.bfloat16):
    result = spread * jax.random.normal(own_key, extent, jnp.float32)
    if cuts:
        result = result * steps_of(own_key, extent, cuts, -0.22, 0.18)
    return jnp.clip(strengthened(result, jax.random.fold_in(own_key, 3), *heavy), -limit, limit).astype(kind)


def setup_inputs(seed: int = 0) -> dict:
    splits = jax.random.split(jax.random.key(seed), 5)
    normed_input = heavy_noise(splits[0], (TOKENS, D), 1.0, 6.0, ((0, 16), (1, 2)), (0, 1, 16, 2.0))
    cotangent = heavy_noise(splits[1], (TOKENS, D), 1.0, 6.0, ((0, 16), (1, 2)), (0, 1, 16, 2.0))
    up_weight = bell_draw(splits[2], (D, FF), D ** -0.5, 0.125, ((0, 16), (1, 2)))
    down_weight = bell_draw(splits[3], (FF, D), FF ** -0.5, 0.0625, ((0, 2), (1, 16)))
    return {"normed_input": normed_input, "cotangent": cotangent, "up_weight": up_weight, "down_weight": down_weight}


def reference(normed_input, cotangent, up_weight, down_weight):
    tokens = normed_input.shape[0]
    width = FF // FF_BLOCKS
    scale = lax.rsqrt(jnp.asarray(tokens, jnp.float32))

    def block(total, index):
        start = (index * width).astype(jnp.int32)
        up_block = lax.dynamic_slice_in_dim(up_weight, start, width, 1)
        down_block = lax.dynamic_slice_in_dim(down_weight, start, width, 0)
        pre = jnp.dot(normed_input, up_block, preferred_element_type=jnp.float32)
        rectified = jax.nn.relu(pre)
        act = (rectified * rectified).astype(jnp.bfloat16)
        act_grad = jnp.dot(cotangent, down_block.T, preferred_element_type=jnp.float32)
        pre_grad = (2.0 * rectified * act_grad).astype(jnp.bfloat16)
        down_part = jnp.dot(act.T, cotangent, preferred_element_type=jnp.float32) * scale
        up_part = jnp.dot(normed_input.T, pre_grad, preferred_element_type=jnp.float32) * scale
        partial_value = jnp.dot(pre_grad, up_block.T, preferred_element_type=jnp.float32).astype(jnp.bfloat16)
        partial_value = lax.optimization_barrier(partial_value)
        return (total + partial_value.astype(jnp.float32), (up_part, down_part))
    start_total = jnp.zeros(normed_input.shape, jnp.float32)
    total, parts = lax.scan(block, start_total, jnp.arange(FF_BLOCKS, dtype=jnp.int32))
    up_parts, down_parts = parts
    up_grad = jnp.moveaxis(up_parts, 0, 1).reshape(D, FF)
    down_grad = down_parts.reshape(FF, D)
    return (total.astype(jnp.bfloat16), up_grad, down_grad)
```

```python
import jax
import jax.numpy as jnp
from jax import lax
from jax.sharding import Mesh, PartitionSpec as P


def hidden_ways(size):
    return 4 if size % 4 == 0 and size > 4 else 1


def right_product(left, right):
    return lax.dot_general(
        left, right, (((1,), (1,)), ((), ())), preferred_element_type=jnp.float32
    )


def left_product(left, right):
    return lax.dot_general(
        left, right, (((0,), (0,)), ((), ())), preferred_element_type=jnp.float32
    )


def swap(array, k):
    ways = lax.axis_size("hid")
    return lax.ppermute(array, "hid", [(i, i ^ k) for i in range(ways)])


def gather_tokens(array):
    ways = lax.axis_size("hid")
    pieces = [array] + [swap(array, k) for k in range(1, ways)]
    array = jnp.concatenate(pieces, axis=0)
    return lax.all_gather(array, "tp", axis=1, tiled=True)


def scatter_tokens(array):
    ways = lax.axis_size("hid")
    pieces = jnp.split(array, ways, axis=0)
    total = pieces[0].astype(jnp.float32)
    for k in range(1, ways):
        total = total + swap(pieces[k], k).astype(jnp.float32)
    return total.astype(array.dtype)


def exchange(blocks):
    ways, me = lax.axis_size("hid"), lax.axis_index("hid")
    got = []
    for k in range(ways):
        block = lax.dynamic_index_in_dim(blocks, me ^ k, 0, keepdims=False)
        got.append(swap(block, k) if k else block)
    got = jnp.stack(got)
    return [
        lax.dynamic_index_in_dim(got, me ^ j, 0, keepdims=False) for j in range(ways)
    ]


def weight_columns(shard):
    ways = lax.axis_size("hid")
    depth, width = shard.shape
    blocks = jnp.moveaxis(shard.reshape(depth, ways, width // ways), 1, 0)
    return jnp.concatenate(exchange(blocks), axis=0)


def scatter_grad(term):
    ways = lax.axis_size("hid")
    width = term.shape[1]
    term = lax.psum_scatter(term, "tok", scatter_dimension=0, tiled=True)
    return jnp.concatenate(exchange(term.reshape(ways, -1, width)), axis=1)


def per_device(normed_input, cotangent, up_weight, down_weight):
    tokens = normed_input.shape[0] * lax.axis_size("tok") * lax.axis_size("hid")
    scale = lax.rsqrt(jnp.asarray(tokens, jnp.float32))
    up_rows = weight_columns(up_weight)
    down_rows = weight_columns(down_weight.T)
    up_rows, down_rows, normed_input, cotangent = lax.optimization_barrier(
        (up_rows, down_rows, normed_input, cotangent)
    )
    block_up = lax.all_gather(up_rows, "tok", axis=0, tiled=True)
    block_down = lax.all_gather(down_rows, "tok", axis=0, tiled=True)
    whole_input = gather_tokens(normed_input)
    whole_cot = gather_tokens(cotangent)
    pre = jnp.dot(whole_input, block_up, preferred_element_type=jnp.float32)
    rectified = jax.nn.relu(pre)
    act = (rectified * rectified).astype(jnp.bfloat16)
    down_term = left_product(whole_cot, act) * scale
    down_grad = scatter_grad(down_term.astype(jnp.bfloat16)).astype(jnp.float32).T
    act_grad = jnp.dot(whole_cot, block_down, preferred_element_type=jnp.float32)
    pre_grad = (2.0 * rectified * act_grad).astype(jnp.bfloat16)
    up_term = left_product(whole_input, pre_grad) * scale
    up_grad = scatter_grad(up_term.astype(jnp.bfloat16)).astype(jnp.float32)
    partial_value = right_product(pre_grad, block_up).astype(jnp.bfloat16)
    input_grad = lax.psum_scatter(
        partial_value, "tp", scatter_dimension=1, tiled=True
    )
    input_grad = scatter_tokens(input_grad)
    return (input_grad, up_grad, down_grad)


def solution(mesh):
    fs, tp = mesh.shape["fs"], mesh.shape["tp"]
    ways = hidden_ways(fs)
    fine = Mesh(
        mesh.devices.reshape(fs // ways, ways, tp), ("tok", "hid", "tp")
    )
    rows = ("tok", "hid")
    in_specs = (P(rows, "tp"), P(rows, "tp"), P(rows, "tp"), P("tp", rows))
    out_specs = (P(rows, "tp"), P(rows, "tp"), P("tp", rows))
    return jax.shard_map(
        per_device, mesh=fine, in_specs=in_specs, out_specs=out_specs, check_vma=False
    )
```
